32 devices in a mesh: sp: 8 (over z, x), tp: 4 (over y, core).
Axes of the slice: x: 2, y: 2, z: 4, core: 2. Of those that a mesh axis runs over, the one named last changes fastest.
Arguments:
- tokens: bfloat16 [3072, 2048], P(('sp', 'tp')), may hold values from -6 to 6
- norm_gain: bfloat16 [2048], replicated, may hold values from 0.099609375 to 1.8984375
- query_down_weight: bfloat16 [2048, 512], replicated, may hold values from -0.125 to 0.125
- query_latent_norm_gain: bfloat16 [512], replicated, may hold values from 0.099609375 to 1.8984375
- key_value_down_weight: bfloat16 [2048, 256], replicated, may hold values from -0.125 to 0.125
- key_value_latent_gain: bfloat16 [256], replicated, may hold values from 0.099609375 to 1.8984375
- w_rope_key: bfloat16 [2048, 32], replicated, may hold values from -0.125 to 0.125
- w_pool_in: bfloat16 [2048, 512], replicated, may hold values from -0.125 to 0.125
- query_up_weight: bfloat16 [512, 2304], P(None, 'tp'), may hold values from -0.25 to 0.25
- key_value_up_weight: bfloat16 [256, 3072], P(None, 'tp'), may hold values from -0.375 to 0.375
- query_gain: bfloat16 [96], replicated, may hold values from 1 to 16
- key_gain: bfloat16 [96], replicated, may hold values from 1 to 16
- w_pool_mix: bfloat16 [8, 64, 64], P('tp'), may hold values from -0.75 to 0.75
- pool_scale: bfloat16 [512], P('tp'), may hold values from 1 to 10
- w_out_attn: bfloat16 [1536, 2048], P('tp'), may hold values from -0.3125 to 0.3125
- w_out_pool: bfloat16 [512, 2048], P('tp'), may hold values from -0.25 to 0.25
Outputs:
- mixed: bfloat16 [3072, 2048], P(('sp', 'tp'))
- row_logsum: float32 [24, 3072], P('tp', 'sp')
The draws below stay inside these ranges and needn't reach their ends.
All inputs are finite; a program needn't handle non-finite values.
Results may differ from the reference program's by a relative error of at most 0.035.
Values may be sent and summed in bfloat16 or wider, within the bound.
A program may use at most 128 MiB of HBM per device.

```python
import math
import jax
import jax.numpy as jnp
from jax import lax

MODEL_WIDTH = 2048
HEAD_COUNT = 24
PLAIN_HEAD_SIZE = 64
ROTARY_SIZE = 32
VALUE_HEAD_SIZE = 64
QUERY_RANK = 512
KEY_VALUE_RANK = 256
GROUPS = 8
GDIM = 64
TOKENS = 3072
N_TP = 4


def head_gain(key, salt):
    base = jax.random.uniform(jax.random.fold_in(key, salt), (PLAIN_HEAD_SIZE + ROTARY_SIZE,), jnp.float32, 1.0, 2.0)
    return base.astype(jnp.bfloat16)


def draw_query_gain(key, part):
    return head_gain(key, 1)


def draw_key_gain(key, part):
    return head_gain(key, 2)


def levels(rng, shape, split, least, high):
    level, own = 1.0, jax.random.fold_in(rng, 6)
    for dim, parts in split:
        draws = jnp.exp(jax.random.uniform(jax.random.fold_in(own, dim), (parts,), jnp.float32, least / len(split), high / len(split)))
        level = level * jnp.repeat(draws, shape[dim] // parts).reshape([-1 if axis == dim else 1 for axis in range(len(shape))])
    return level


def noise(rng, shape, spread, limit, split=(), held_as=jnp.bfloat16):
    level = levels(rng, shape, split, -0.22, 0.18) if split else 1.0
    values = jax.random.normal(rng, shape, jnp.float32) * spread * level
    return jnp.minimum(jnp.maximum(values, -limit), limit).astype(held_as)


def setup_inputs(seed: int = 0) -> dict:
    arg_keys = jax.random.split(jax.random.key(seed), 17)
    return {
        "tokens": noise(arg_keys[0], (TOKENS, MODEL_WIDTH), 1.0, 6.0, ((0, 32),)),
        "norm_gain": jnp.clip(1.0 + 0.18 * jax.random.normal(arg_keys[1], (MODEL_WIDTH,), jnp.float32), 0.099609375, 1.8984375).astype(jnp.bfloat16),
        "query_down_weight": noise(arg_keys[2], (MODEL_WIDTH, QUERY_RANK), MODEL_WIDTH ** -0.5, 0.125),
        "query_latent_norm_gain": jnp.clip(1.0 + 0.18 * jax.random.normal(arg_keys[3], (QUERY_RANK,), jnp.float32), 0.099609375, 1.8984375).astype(jnp.bfloat16),
        "key_value_down_weight": noise(arg_keys[4], (MODEL_WIDTH, KEY_VALUE_RANK), MODEL_WIDTH ** -0.5, 0.125),
        "key_value_latent_gain": jnp.clip(1.0 + 0.18 * jax.random.normal(arg_keys[5], (KEY_VALUE_RANK,), jnp.float32), 0.099609375, 1.8984375).astype(jnp.bfloat16),
        "w_rope_key": noise(arg_keys[6], (MODEL_WIDTH, ROTARY_SIZE), MODEL_WIDTH ** -0.5, 0.125),
        "w_pool_in": noise(arg_keys[7], (MODEL_WIDTH, GROUPS * GDIM), MODEL_WIDTH ** -0.5, 0.125),
        "query_up_weight": noise(arg_keys[8], (QUERY_RANK, HEAD_COUNT * (PLAIN_HEAD_SIZE + ROTARY_SIZE)), QUERY_RANK ** -0.5, 0.25, ((1, 4),)),
        "key_value_up_weight": noise(arg_keys[9], (KEY_VALUE_RANK, HEAD_COUNT * (PLAIN_HEAD_SIZE + VALUE_HEAD_SIZE)), KEY_VALUE_RANK ** -0.5, 0.375, ((1, 4),)),
        "query_gain": draw_query_gain(jax.random.fold_in(arg_keys[16], 71), 0),
        "key_gain": draw_key_gain(jax.random.fold_in(arg_keys[16], 71), 0),
        "w_pool_mix": noise(arg_keys[12], (GROUPS, GDIM, GDIM), GDIM ** -0.5, 0.75, ((0, 4),)),
        "pool_scale": jnp.clip(jnp.exp(math.log(10.0) - 2.3025851 * jax.random.uniform(arg_keys[13], (GROUPS * GDIM,), jnp.float32) ** levels(arg_keys[13], (GROUPS * GDIM,), ((0, 4),), -0.2, 0.2)), 1.0, 10.0).astype(jnp.bfloat16),
        "w_out_attn": noise(arg_keys[14], (HEAD_COUNT * VALUE_HEAD_SIZE, MODEL_WIDTH), (HEAD_COUNT * VALUE_HEAD_SIZE // 4) ** -0.5, 0.3125, ((0, 4),)),
        "w_out_pool": noise(arg_keys[15], (GROUPS * GDIM, MODEL_WIDTH), (GROUPS * GDIM) ** -0.5, 0.25, ((0, 4),)),
    }


epsilon = 1e-06
rope_base = 10000.0
query_rows = 128

def norm_rows(values, gain):
    mean_square = lax.optimization_barrier(jnp.mean(values * values, axis=-1, keepdims=True))
    return values * lax.rsqrt(mean_square + epsilon) * gain.astype(jnp.float32)

def rotate_tail(values, positions):
    half = ROTARY_SIZE // 2
    freqs = rope_base ** (-jnp.arange(half, dtype=jnp.float32) / half)
    angles = positions[:, None] * freqs[None, :]
    cosine = jnp.cos(angles)[:, None, :]
    sine = jnp.sin(angles)[:, None, :]
    first = values[..., PLAIN_HEAD_SIZE:PLAIN_HEAD_SIZE + half]
    second = values[..., PLAIN_HEAD_SIZE + half:]
    return jnp.concatenate([values[..., :PLAIN_HEAD_SIZE], first * cosine - second * sine, first * sine + second * cosine], axis=-1)

def reference(tokens, norm_gain, query_down_weight, query_latent_norm_gain, key_value_down_weight, key_value_latent_gain, w_rope_key, w_pool_in, query_up_weight, key_value_up_weight, query_gain, key_gain, w_pool_mix, pool_scale, w_out_attn, w_out_pool):
    length = tokens.shape[0]
    normed = norm_rows(tokens.astype(jnp.float32), norm_gain).astype(jnp.bfloat16)
    query_latent = norm_rows(jnp.dot(normed, query_down_weight, preferred_element_type=jnp.float32), query_latent_norm_gain).astype(jnp.bfloat16)
    kv_latent = norm_rows(jnp.dot(normed, key_value_down_weight, preferred_element_type=jnp.float32), key_value_latent_gain).astype(jnp.bfloat16)
    rope_key = jnp.dot(normed, w_rope_key, preferred_element_type=jnp.float32).astype(jnp.bfloat16)
    pool_input = jnp.dot(normed, w_pool_in, preferred_element_type=jnp.float32).astype(jnp.bfloat16)
    positions = jnp.arange(length, dtype=jnp.int32).astype(jnp.float32)
    query_vectors = jnp.dot(query_latent, query_up_weight, preferred_element_type=jnp.float32).reshape(length, HEAD_COUNT, PLAIN_HEAD_SIZE + ROTARY_SIZE)
    query_vectors = rotate_tail(norm_rows(query_vectors, query_gain), positions).astype(jnp.bfloat16)
    key_value_pair = jnp.dot(kv_latent, key_value_up_weight, preferred_element_type=jnp.float32).reshape(length, HEAD_COUNT, PLAIN_HEAD_SIZE + VALUE_HEAD_SIZE)
    shared = jnp.broadcast_to(rope_key.astype(jnp.float32)[:, None, :], (length, HEAD_COUNT, ROTARY_SIZE))
    keys = jnp.concatenate([key_value_pair[..., :PLAIN_HEAD_SIZE], shared], axis=-1)
    keys = rotate_tail(norm_rows(keys, key_gain), positions).astype(jnp.bfloat16)
    values = key_value_pair[..., PLAIN_HEAD_SIZE:].astype(jnp.bfloat16)
    scale = (PLAIN_HEAD_SIZE + ROTARY_SIZE) ** (-0.5)
    key_float = keys.astype(jnp.float32)
    value_float = values.astype(jnp.float32)
    query_blocks = query_vectors.astype(jnp.float32).reshape(length // query_rows, query_rows, HEAD_COUNT, PLAIN_HEAD_SIZE + ROTARY_SIZE)

    def attend(query_block):
        scores = jnp.einsum('qhd,khd->hqk', query_block, key_float) * scale
        row_max = lax.optimization_barrier(jnp.max(scores, axis=-1))
        exp_scores = jnp.exp(scores - row_max[:, :, None])
        row_total = lax.optimization_barrier(jnp.sum(exp_scores, axis=-1))
        weights = lax.optimization_barrier(exp_scores.astype(jnp.bfloat16)).astype(jnp.float32)
        summed = jnp.einsum('hqk,khd->qhd', weights, value_float)
        output = (summed / jnp.transpose(row_total)[:, :, None]).astype(jnp.bfloat16)
        return (output, row_max + jnp.log(row_total))
    outputs, logsums = lax.map(attend, query_blocks)
    attention = outputs.reshape(length, HEAD_COUNT * VALUE_HEAD_SIZE)
    row_logsum = jnp.transpose(logsums, (1, 0, 2)).reshape(HEAD_COUNT, length)
    pool_float = pool_input.astype(jnp.float32)
    running = jnp.concatenate([jnp.zeros((1, GROUPS * GDIM), jnp.float32), jnp.cumsum(pool_float, axis=0)], axis=0)
    places = jnp.arange(length, dtype=jnp.int32)
    pieces = []
    for group in range(GROUPS):
        half = 2 ** (group % 4)
        upper = jnp.minimum(places + half, length)
        lower = jnp.maximum(places - half, 0)
        first_col = group * GDIM
        window = running[upper, first_col:first_col + GDIM] - running[lower, first_col:first_col + GDIM]
        total_count = (upper - lower).astype(jnp.float32)[:, None]
        pooled = (window / total_count - pool_float[:, first_col:first_col + GDIM]).astype(jnp.bfloat16)
        mapped = jnp.dot(pooled, w_pool_mix[group], preferred_element_type=jnp.float32)
        pieces.append((mapped * pool_scale[first_col:first_col + GDIM].astype(jnp.float32)).astype(jnp.bfloat16))
    pool_out = jnp.concatenate(pieces, axis=1)
    head_cols = HEAD_COUNT * VALUE_HEAD_SIZE // N_TP
    pool_cols = GROUPS * GDIM // N_TP
    mixed = jnp.zeros((length, MODEL_WIDTH), jnp.float32)
    for member in range(N_TP):
        head_start = member * head_cols
        pool_start = member * pool_cols
        partial_sum = jnp.dot(attention[:, head_start:head_start + head_cols], w_out_attn[head_start:head_start + head_cols], preferred_element_type=jnp.float32)
        partial_sum = partial_sum + jnp.dot(pool_out[:, pool_start:pool_start + pool_cols], w_out_pool[pool_start:pool_start + pool_cols], preferred_element_type=jnp.float32)
        mixed = mixed + lax.optimization_barrier(partial_sum.astype(jnp.bfloat16)).astype(jnp.float32)
    return (mixed.astype(jnp.bfloat16), row_logsum)
```

```python
import functools

import jax
import jax.numpy as jnp
import numpy as np
from jax import lax
from jax.experimental import pallas as pl
from jax.experimental.pallas import tpu as pltpu
from jax.sharding import PartitionSpec as P

PLAIN = 64
ROT = 32
HEAD = PLAIN + ROT
VALUE = 64
GDIM = 64
EPS = 1e-06
ROPE_BASE = 10000.0
HALO = 16
F32 = jnp.float32
BF16 = jnp.bfloat16
MESH = pl.DeviceIdType.MESH
VMEM = pl.BlockSpec(memory_space=pltpu.VMEM)


def rms(x, width):
    return lax.rsqrt(jnp.sum(x * x, axis=-1, keepdims=True) * (1.0 / width) + EPS)


def mm(a, b):
    return jnp.dot(a, b, preferred_element_type=F32)


def gather_kernel(n_sp, n_tp, x_ref, gain_ref, wq_ref, qg_ref, wkv_ref, kvg_ref, wr_ref, wp_ref,
                  q_ref, pool_ref, kv_ref, pool_src,
                  kv_send, kv_recv, part_send, q_send, q_recv, p_send, p_recv, h_send, h_recv):
    sp = lax.axis_index("sp")
    tp = lax.axis_index("tp")
    n_dev = n_sp * n_tp
    n_ty = n_tp // 2
    n_chip = n_sp * n_ty
    me = sp * n_tp + tp
    core = lax.rem(tp, 2)
    ty = tp // 2
    partner = ty * 2 + 1 - core
    rows = x_ref.shape[0]
    pool_cols = pool_ref.shape[1]
    barrier = pltpu.get_barrier_semaphore()

    @pl.loop(1, n_dev)
    def _(i):
        d = lax.rem(me + i, n_dev)
        pl.semaphore_signal(barrier, inc=1, device_id=(d // n_tp, lax.rem(d, n_tp)), device_id_type=MESH)

    x = x_ref[...].astype(F32)
    normed = (x * rms(x, x.shape[1]) * gain_ref[...].astype(F32)).astype(BF16)
    kv = mm(normed, wkv_ref[...])
    kv_ref[me, :rows, :] = (kv * rms(kv, kv.shape[1]) * kvg_ref[...].astype(F32)).astype(BF16)
    rope = mm(normed, wr_ref[...])
    groups = rows // 16
    packed = [rope[16 * j : 16 * j + 16, :] for j in range(groups)]
    packed.append(jnp.zeros((16, kv.shape[1] - groups * ROT), F32))
    kv_ref[me, rows:, :] = jnp.concatenate(packed, axis=1).astype(BF16)
    pl.semaphore_wait(barrier, n_dev - 1)

    def chip_of(i):
        s = lax.rem(sp + i // n_ty, n_sp)
        t = lax.rem(ty + lax.rem(i, n_ty), n_ty) * 2 + core
        return s, t

    def source_of(i):
        s = lax.rem(sp + n_sp - i // n_ty, n_sp)
        t = lax.rem(ty + n_ty - lax.rem(i, n_ty), n_ty) * 2 + core
        return s * n_tp + t

    def kv_copy(slot, send_sem, target):
        return pltpu.make_async_remote_copy(
            src_ref=kv_ref.at[slot], dst_ref=kv_ref.at[slot], send_sem=send_sem,
            recv_sem=kv_recv.at[slot], device_id=target, device_id_type=MESH)

    @pl.loop(1, n_chip)
    def _(i):
        kv_copy(me, kv_send.at[i], chip_of(i)).start()

    kv_copy(me, part_send.at[0], (sp, partner)).start()

    q = mm(normed, wq_ref[...])
    q_rows = pl.ds(pl.multiple_of(tp * rows, 16), rows)
    q_ref[q_rows, :] = (q * rms(q, q.shape[1]) * qg_ref[...].astype(F32)).astype(BF16)

    def q_copy(i):
        return pltpu.make_async_remote_copy(
            src_ref=q_ref.at[q_rows], dst_ref=q_ref.at[q_rows], send_sem=q_send.at[i],
            recv_sem=q_recv.at[i], device_id=(sp, lax.rem(tp + i, n_tp)), device_id_type=MESH)

    for i in range(1, n_tp):
        q_copy(i).start()
    pool = mm(normed, wp_ref[...]).astype(BF16)
    for t in range(n_tp):
        pool_src[t] = pool[:, t * pool_cols : (t + 1) * pool_cols]
    pool_ref[pl.ds(pl.multiple_of(HALO + tp * rows, 16), rows), :] = pool_src[tp]

    def p_copy(i):
        t = lax.rem(tp + i, n_tp)
        return pltpu.make_async_remote_copy(
            src_ref=pool_src.at[t],
            dst_ref=pool_ref.at[pl.ds(pl.multiple_of(HALO + tp * rows, 16), rows)],
            send_sem=p_send.at[i], recv_sem=p_recv.at[i],
            device_id=(sp, t), device_id_type=MESH)

    for i in range(1, n_tp):
        p_copy(i).start()
    last = HALO + n_tp * rows

    def up_copy(t):
        return pltpu.make_async_remote_copy(
            src_ref=pool_src.at[t, pl.ds(rows - HALO, HALO)], dst_ref=pool_ref.at[pl.ds(0, HALO)],
            send_sem=h_send.at[t], recv_sem=h_recv.at[0], device_id=(sp + 1, t), device_id_type=MESH)

    def down_copy(t):
        return pltpu.make_async_remote_copy(
            src_ref=pool_src.at[t, pl.ds(0, HALO)], dst_ref=pool_ref.at[pl.ds(last, HALO)],
            send_sem=h_send.at[n_tp + t], recv_sem=h_recv.at[1], device_id=(sp - 1, t), device_id_type=MESH)

    sends_up = jnp.logical_and(tp == n_tp - 1, sp < n_sp - 1)
    sends_down = jnp.logical_and(tp == 0, sp > 0)

    @pl.when(sends_up)
    def _():
        for t in range(n_tp):
            up_copy(t).start()

    @pl.when(sends_down)
    def _():
        for t in range(n_tp):
            down_copy(t).start()

    @pl.when(sp == 0)
    def _():
        pool_ref[:HALO, :] = jnp.zeros((HALO, pool_cols), BF16)

    @pl.when(sp == n_sp - 1)
    def _():
        pool_ref[last:, :] = jnp.zeros((HALO, pool_cols), BF16)

    @pl.loop(1, n_chip)
    def _(i):
        slot = source_of(i)
        kv_copy(slot, part_send.at[i], (sp, partner)).wait_recv()
        kv_copy(slot, part_send.at[i], (sp, partner)).start()

    @pl.loop(0, n_chip)
    def _(i):
        slot = source_of(i) - core + 1 - core
        kv_copy(slot, part_send.at[i], (sp, partner)).wait_recv()

    for i in range(1, n_tp):
        q_copy(i).wait()
        p_copy(i).wait()

    @pl.when(sp > 0)
    def _():
        pltpu.make_async_remote_copy(
            src_ref=pool_src.at[0, pl.ds(0, HALO)], dst_ref=pool_ref.at[pl.ds(0, HALO)],
            send_sem=h_send.at[0], recv_sem=h_recv.at[0], device_id=(sp, partner), device_id_type=MESH).wait_recv()

    @pl.when(sp < n_sp - 1)
    def _():
        pltpu.make_async_remote_copy(
            src_ref=pool_src.at[0, pl.ds(0, HALO)], dst_ref=pool_ref.at[pl.ds(last, HALO)],
            send_sem=h_send.at[0], recv_sem=h_recv.at[1], device_id=(sp, partner), device_id_type=MESH).wait_recv()

    @pl.when(sends_up)
    def _():
        for t in range(n_tp):
            up_copy(t).wait_send()

    @pl.when(sends_down)
    def _():
        for t in range(n_tp):
            down_copy(t).wait_send()

    @pl.loop(1, n_chip)
    def _(i):
        kv_copy(me, kv_send.at[i], chip_of(i)).wait_send()

    @pl.loop(0, n_chip)
    def _(i):
        kv_copy(me, part_send.at[i], (sp, partner)).wait_send()


def turn(y, cosine, sine, lane):
    half = ROT // 2
    width = y.shape[-1]
    swapped = jnp.where(lane < PLAIN + half, pltpu.roll(y, width - half, 1), pltpu.roll(y, half, 1))
    return y * cosine + swapped * sine


def mixer_kernel(n_sp, n_tp, q_ref, pool_ref, kv_ref, wqu_ref, wkvu_ref, qg_ref, kg_ref, mix_ref, scale_ref,
                 woa_ref, wop_ref, base_ref, block_ref,
                 out_ref, lse_ref, q_s, k_s, v_s, cat_s):
    sp = lax.axis_index("sp")
    tp = lax.axis_index("tp")
    rows = q_ref.shape[0]
    part = rows // n_tp
    heads = wqu_ref.shape[1] // HEAD
    pairs = q_s.shape[0] // 2
    rank = kv_ref.shape[2]
    lane = lax.broadcasted_iota(jnp.int32, (rows, 128), 1)

    def table(b):
        ca, sa = base_ref[:, :128], base_ref[:, 128:]
        cb, sb = block_ref[b, :, :128], block_ref[b, :, 128:]
        return ca * cb - sa * sb, sa * cb + ca * sb

    cq, sq = table(sp)
    qg = qg_ref[...]
    ql = q_ref[...]
    for h in range(heads):
        w = jnp.concatenate(
            [wqu_ref[:, h * HEAD : (h + 1) * HEAD], jnp.zeros((wqu_ref.shape[0], 128 - HEAD), BF16)], axis=1)
        y = mm(ql, w)
        q_s[h] = turn(y * rms(y, HEAD) * qg, cq, sq, lane).astype(BF16)

    for h in range(heads, 2 * pairs):
        q_s[h] = jnp.zeros(q_s.shape[1:], BF16)

    kg = kg_ref[...]

    @pl.loop(0, n_sp)
    def _(b):
        lat = jnp.concatenate([kv_ref[b * n_tp + t, :part, :] for t in range(n_tp)], axis=0)
        pieces = []
        for t in range(n_tp):
            packed = kv_ref[b * n_tp + t, part:, :].astype(F32)
            for j in range(part // 16):
                pieces.append(packed[:, j * ROT : (j + 1) * ROT])
        rope = jnp.concatenate(pieces, axis=0)
        rope = jnp.concatenate([jnp.zeros((rows, PLAIN), F32), rope, jnp.zeros((rows, 128 - HEAD), F32)], axis=1)
        rope_sum = jnp.sum(rope * rope, axis=-1, keepdims=True)
        ck, sk = table(b)
        rotated = turn(rope * kg, ck, sk, lane)
        pair = mm(lat, wkvu_ref[...])
        at = pl.ds(pl.multiple_of(b * rows, 128), rows)
        for h in range(heads):
            kvh = pair[:, h * 128 : (h + 1) * 128]
            plain = jnp.where(lane < PLAIN, kvh, 0.0)
            r = lax.rsqrt((jnp.sum(plain * plain, axis=-1, keepdims=True) + rope_sum) * (1.0 / HEAD) + EPS)
            k_s[h, at, :] = (jnp.where(lane < PLAIN, kvh * kg, rotated) * r).astype(BF16)
            v_s[h, at, :] = jnp.where(lane < PLAIN, 1.0, kvh).astype(BF16)
        for h in range(heads, 2 * pairs):
            k_s[h, at, :] = jnp.zeros((rows, 128), BF16)
            v_s[h, at, :] = jnp.ones((rows, 128), BF16)

    chunk = 128
    lane_c = lax.broadcasted_iota(jnp.int32, (chunk, 128), 1)

    def one_head(h, at):
        s = lax.dot_general(q_s[h, at, :], k_s[h], (((1,), (1,)), ((), ())), preferred_element_type=F32)
        m = jnp.max(s, axis=-1, keepdims=True)
        p = jnp.exp2(s - m).astype(BF16)
        o = mm(p, v_s[h])
        total = o[:, :1]
        lse = m * np.float32(np.log(2.0)) + jnp.log(total)
        return o * (1.0 / total), lse

    @pl.loop(0, rows // chunk)
    def _(c):
        at = pl.ds(pl.multiple_of(c * chunk, chunk), chunk)

        @pl.loop(0, pairs)
        def _(j):
            even, lse0 = one_head(2 * j, at)
            odd, lse1 = one_head(2 * j + 1, at)
            both = jnp.where(lane_c < VALUE, pltpu.roll(even, VALUE, 1), odd)
            cat_s[j, at, :] = both.astype(BF16)
            two = jnp.concatenate([lse0, lse1], axis=1)
            lse_ref[pl.ds(j, 1), :, at] = jnp.transpose(two)[None]

    x = pool_ref[...].astype(F32)
    size = x.shape[0]
    w1 = x + pltpu.roll(x, 1, 0)
    w2 = pltpu.roll(w1, 1, 0) + pltpu.roll(w1, size - 1, 0)
    w4 = pltpu.roll(w2, 2, 0) + pltpu.roll(w2, size - 2, 0)
    w8 = pltpu.roll(w4, 4, 0) + pltpu.roll(w4, size - 4, 0)
    x, w1, w2, w4, w8 = (v[HALO : HALO + rows] for v in (x, w1, w2, w4, w8))
    groups_here = mix_ref.shape[0]
    wide = x.shape[1]
    kind = lax.rem(tp * groups_here + lane[:, :wide] // GDIM, 4)
    window = jnp.where(kind == 0, w1, jnp.where(kind == 1, w2, jnp.where(kind == 2, w4, w8)))
    half = jnp.where(kind == 0, 1, jnp.where(kind == 1, 2, jnp.where(kind == 2, 4, 8)))
    place = sp * rows + lax.broadcasted_iota(jnp.int32, (rows, wide), 0)
    count = (jnp.minimum(place + half, rows * n_sp) - jnp.maximum(place - half, 0)).astype(F32)
    pooled = (window / count - x).astype(BF16)
    mapped = jnp.concatenate(
        [mm(pooled[:, g * GDIM : (g + 1) * GDIM], mix_ref[g]) for g in range(groups_here)], axis=1)
    pool_out = (mapped * scale_ref[...].astype(F32)).astype(BF16)
    attention = jnp.concatenate([cat_s[j] for j in range(pairs)], axis=1)[:, : heads * VALUE]
    tile = 512

    @pl.loop(0, out_ref.shape[1] // tile)
    def _(i):
        cols = pl.ds(pl.multiple_of(i * tile, tile), tile)
        out_ref[:, cols] = (mm(attention, woa_ref[:, cols]) + mm(pool_out, wop_ref[:, cols])).astype(BF16)


def scatter_kernel(n_tp, pieces, x_ref, out_ref, from_partner, to_send, from_chip, d_send, d_recv, c_send, c_recv):
    sp = lax.axis_index("sp")
    tp = lax.axis_index("tp")
    n_ty = n_tp // 2
    core = lax.rem(tp, 2)
    ty = tp // 2
    partner = ty * 2 + 1 - core
    rows = out_ref.shape[0]
    width = out_ref.shape[1] // pieces
    barrier = pltpu.get_barrier_semaphore()
    for i in range(1, n_tp):
        pl.semaphore_signal(barrier, inc=1, device_id=(sp, lax.rem(tp + i, n_tp)), device_id_type=MESH)
    pl.semaphore_wait(barrier, n_tp - 1)

    def cols(p):
        return pl.ds(p * width, width)

    def at(i, c):
        return pl.ds(pl.multiple_of((lax.rem(ty + i, n_ty) * 2 + c) * rows, 16), rows)

    def d_copy(i, p):
        return pltpu.make_async_remote_copy(
            src_ref=x_ref.at[at(i, 1 - core), cols(p)], dst_ref=from_partner.at[i, :, cols(p)],
            send_sem=d_send.at[i * pieces + p], recv_sem=d_recv.at[i * pieces + p],
            device_id=(sp, partner), device_id_type=MESH)

    def c_copy(i, p):
        return pltpu.make_async_remote_copy(
            src_ref=to_send.at[i, :, cols(p)], dst_ref=from_chip.at[i, :, cols(p)],
            send_sem=c_send.at[i * pieces + p], recv_sem=c_recv.at[i * pieces + p],
            device_id=(sp, lax.rem(ty + i, n_ty) * 2 + core), device_id_type=MESH)

    order = [(i, p) for i in list(range(1, n_ty)) + [0] for p in range(pieces)]
    for i, p in order:
        d_copy(i, p).start()
    for i, p in order:
        if i:
            d_copy(i, p).wait_recv()
            to_send[i, :, cols(p)] = (
                x_ref[at(i, core), cols(p)].astype(F32) + from_partner[i, :, cols(p)].astype(F32)).astype(BF16)
            c_copy(i, p).start()
    for p in range(pieces):
        d_copy(0, p).wait_recv()
        total = x_ref[at(0, core), cols(p)].astype(F32) + from_partner[0, :, cols(p)].astype(F32)
        for i in range(1, n_ty):
            c_copy(i, p).wait_recv()
            total = total + from_chip[i, :, cols(p)].astype(F32)
        out_ref[:, cols(p)] = total.astype(BF16)
    for i, p in order:
        d_copy(i, p).wait_send()
        if i:
            c_copy(i, p).wait_send()


def tables(rows, blocks):
    half = ROT // 2
    freqs = ROPE_BASE ** (-np.arange(half, dtype=np.float64) / half)

    def make(positions):
        angle = positions[:, None] * freqs[None, :]
        out = np.zeros((len(positions), 256), np.float64)
        out[:, :PLAIN] = 1.0
        out[:, PLAIN:HEAD] = np.concatenate([np.cos(angle), np.cos(angle)], axis=1)
        out[:, 128 + PLAIN : 128 + HEAD] = np.concatenate([-np.sin(angle), np.sin(angle)], axis=1)
        return out.astype(np.float32)

    return make(np.arange(rows)), make(np.arange(blocks) * rows)[:, None]


def shards(n_sp, n_tp, tokens, norm_gain, wq, q_lat_gain, wkv, kv_lat_gain, w_rope, w_pool_in, wqu, wkvu,
           query_gain, key_gain, w_mix, pool_scale, w_out_attn, w_out_pool):
    rows_own, width = tokens.shape
    rows = rows_own * n_tp
    heads = wqu.shape[1] // HEAD
    pool_cols = w_mix.shape[0] * GDIM
    n_dev = n_sp * n_tp
    n_chip = n_dev // 2
    dma = pltpu.SemaphoreType.DMA
    rank = wkv.shape[1]
    q_lat, pool_in, kvr = pl.pallas_call(
        functools.partial(gather_kernel, n_sp, n_tp),
        out_shape=[
            jax.ShapeDtypeStruct((rows, wq.shape[1]), BF16),
            jax.ShapeDtypeStruct((rows + 2 * HALO, pool_cols), BF16),
            jax.ShapeDtypeStruct((n_dev, rows_own + 16, rank), BF16),
        ],
        in_specs=[VMEM] * 8,
        out_specs=[VMEM] * 3,
        scratch_shapes=[
            pltpu.VMEM((n_tp, rows_own, pool_cols), BF16),
            dma((n_chip,)), dma((n_dev,)), dma((n_chip,)),
            dma((n_tp,)), dma((n_tp,)), dma((n_tp,)), dma((n_tp,)), dma((2 * n_tp,)), dma((2,)),
        ],
        compiler_params=pltpu.CompilerParams(
            collective_id=0, has_side_effects=True, vmem_limit_bytes=60 * 2**20),
    )(tokens, norm_gain[None], wq, q_lat_gain[None], wkv, kv_lat_gain[None], w_rope, w_pool_in)

    base, block = tables(rows, n_sp)
    pad = (0, 128 - HEAD)
    factor = np.float32(HEAD ** -0.5 * np.log2(np.e))
    qg = jnp.pad(query_gain.astype(F32) * factor, pad)[None]
    kg = jnp.pad(key_gain.astype(F32), pad)[None]
    total = rows * n_sp
    pairs = (heads + 1) // 2
    partial, lse = pl.pallas_call(
        functools.partial(mixer_kernel, n_sp, n_tp),
        out_shape=[
            jax.ShapeDtypeStruct((rows, width), BF16),
            jax.ShapeDtypeStruct((pairs, 2, rows), F32),
        ],
        in_specs=[VMEM] * 13,
        out_specs=[VMEM] * 2,
        scratch_shapes=[
            pltpu.VMEM((2 * pairs, rows, 128), BF16),
            pltpu.VMEM((2 * pairs, total, 128), BF16),
            pltpu.VMEM((2 * pairs, total, 128), BF16),
            pltpu.VMEM((pairs, rows, 128), BF16),
        ],
        compiler_params=pltpu.CompilerParams(vmem_limit_bytes=62 * 2**20),
    )(q_lat, pool_in, kvr, wqu, wkvu, qg, kg, w_mix, pool_scale[None], w_out_attn, w_out_pool, base, block)

    pieces = 2
    n_ty = n_tp // 2
    mixed = pl.pallas_call(
        functools.partial(scatter_kernel, n_tp, pieces),
        out_shape=jax.ShapeDtypeStruct((rows_own, width), BF16),
        in_specs=[VMEM],
        out_specs=VMEM,
        scratch_shapes=[
            pltpu.VMEM((n_ty, rows_own, width), BF16),
            pltpu.VMEM((n_ty, rows_own, width), BF16),
            pltpu.VMEM((n_ty, rows_own, width), BF16),
            dma((n_ty * pieces,)), dma((n_ty * pieces,)), dma((n_ty * pieces,)), dma((n_ty * pieces,)),
        ],
        compiler_params=pltpu.CompilerParams(collective_id=1, has_side_effects=True),
    )(partial)
    return mixed, lse.reshape(2 * pairs, rows)[:heads]


def solution(mesh):
    placed = (
        P(("sp", "tp"), None), P(), P(), P(), P(), P(), P(), P(),
        P(None, "tp"), P(None, "tp"), P(), P(),
        P("tp", None, None), P("tp"), P("tp", None), P("tp", None),
    )
    return jax.shard_map(
        functools.partial(shards, mesh.shape["sp"], mesh.shape["tp"]),
        mesh=mesh,
        in_specs=placed,
        out_specs=(P(("sp", "tp"), None), P("tp", "sp")),
        check_vma=False,
    )
```

```python
import functools

import jax
import jax.numpy as jnp
import numpy as np
from jax import lax
from jax.experimental import pallas as pl
from jax.experimental.pallas import tpu as pltpu
from jax.sharding import PartitionSpec as P

PLAIN = 64
ROT = 32
HEAD = PLAIN + ROT
VALUE = 64
GDIM = 64
EPS = 1e-06
ROPE_BASE = 10000.0
HALO = 16
F32 = jnp.float32
BF16 = jnp.bfloat16
MESH = pl.DeviceIdType.MESH
VMEM = pl.BlockSpec(memory_space=pltpu.VMEM)


def rms(x, width):
    return lax.rsqrt(jnp.sum(x * x, axis=-1, keepdims=True) * (1.0 / width) + EPS)


def row(ref, width=None):
    v = ref[...].astype(F32).reshape(1, ref.shape[0])
    if width and width > ref.shape[0]:
        v = jnp.concatenate([v, jnp.zeros((1, width - ref.shape[0]), F32)], axis=1)
    return v


def mm_t(a, b):
    return lax.dot_general(a, b, (((1,), (1,)), ((), ())), preferred_element_type=F32)


def mm(a, b):
    return jnp.dot(a, b, preferred_element_type=F32)


def turn(y, cosine, sine, lane):
    half = ROT // 2
    width = y.shape[-1]
    swapped = jnp.where(lane < PLAIN + half, pltpu.roll(y, width - half, 1), pltpu.roll(y, half, 1))
    return y * cosine + swapped * sine


def layer_kernel(n_sp, n_tp, pieces, x_ref, gain_ref, wq_ref, qlg_ref, wkv_ref, kvg_ref, wr_ref, wp_ref,
                 wqu_ref, wkvu_ref, qg_ref, kg_ref, mix_ref, scale_ref, woa_ref, wop_ref, base_ref, block_ref,
                 out_ref, lse_ref,
                 q_ref, pool_ref, kv_ref, pool_src, q_s, k_s, v_s, cat_s, att_s, part_s, from_partner, to_send, from_chip,
                 kv_send, kv_recv, part_send, q_send, q_recv, p_send, p_recv, h_send, h_recv,
                 d_send, d_recv, c_send, c_recv):
    sp = lax.axis_index("sp")
    tp = lax.axis_index("tp")
    n_dev = n_sp * n_tp
    n_ty = n_tp // 2
    n_chip = n_sp * n_ty
    me = sp * n_tp + tp
    core = lax.rem(tp, 2)
    ty = tp // 2
    partner = ty * 2 + 1 - core
    part = x_ref.shape[0]
    pool_cols = pool_ref.shape[1]
    barrier = pltpu.get_barrier_semaphore()

    @pl.loop(1, n_dev)
    def _(i):
        d = lax.rem(me + i, n_dev)
        pl.semaphore_signal(barrier, inc=1, device_id=(d // n_tp, lax.rem(d, n_tp)), device_id_type=MESH)

    x = x_ref[...].astype(F32)
    normed = (x * rms(x, x.shape[1]) * row(gain_ref)).astype(BF16)
    kv = mm(normed, wkv_ref[...])
    kv_ref[me, :part, :] = (kv * rms(kv, kv.shape[1]) * row(kvg_ref)).astype(BF16)
    rope = mm_t(normed, wr_ref[...])
    groups = part // 16
    packed = [rope[16 * j : 16 * j + 16, :] for j in range(groups)]
    packed.append(jnp.zeros((16, kv.shape[1] - groups * ROT), F32))
    kv_ref[me, part:, :] = jnp.concatenate(packed, axis=1).astype(BF16)
    pl.semaphore_wait(barrier, n_dev - 1)

    def chip_of(i):
        s = lax.rem(sp + i // n_ty, n_sp)
        t = lax.rem(ty + lax.rem(i, n_ty), n_ty) * 2 + core
        return s, t

    def source_of(i):
        s = lax.rem(sp + n_sp - i // n_ty, n_sp)
        t = lax.rem(ty + n_ty - lax.rem(i, n_ty), n_ty) * 2 + core
        return s * n_tp + t

    def kv_copy(slot, send_sem, target):
        return pltpu.make_async_remote_copy(
            src_ref=kv_ref.at[slot], dst_ref=kv_ref.at[slot], send_sem=send_sem,
            recv_sem=kv_recv.at[slot], device_id=target, device_id_type=MESH)

    @pl.loop(1, n_chip)
    def _(i):
        kv_copy(me, kv_send.at[i], chip_of(i)).start()

    kv_copy(me, part_send.at[0], (sp, partner)).start()

    q = mm(normed, wq_ref[...])
    q_rows = pl.ds(pl.multiple_of(tp * part, 16), part)
    q_ref[q_rows, :] = (q * rms(q, q.shape[1]) * row(qlg_ref)).astype(BF16)

    def q_copy(i):
        return pltpu.make_async_remote_copy(
            src_ref=q_ref.at[q_rows], dst_ref=q_ref.at[q_rows], send_sem=q_send.at[i],
            recv_sem=q_recv.at[i], device_id=(sp, lax.rem(tp + i, n_tp)), device_id_type=MESH)

    for i in range(1, n_tp):
        q_copy(i).start()
    pool = mm(normed, wp_ref[...]).astype(BF16)
    for t in range(n_tp):
        pool_src[t] = pool[:, t * pool_cols : (t + 1) * pool_cols]
    pool_ref[pl.ds(pl.multiple_of(HALO + tp * part, 16), part), :] = pool_src[tp]

    def p_copy(i):
        t = lax.rem(tp + i, n_tp)
        return pltpu.make_async_remote_copy(
            src_ref=pool_src.at[t],
            dst_ref=pool_ref.at[pl.ds(pl.multiple_of(HALO + tp * part, 16), part)],
            send_sem=p_send.at[i], recv_sem=p_recv.at[i],
            device_id=(sp, t), device_id_type=MESH)

    for i in range(1, n_tp):
        p_copy(i).start()
    last = HALO + n_tp * part

    def up_copy(t):
        return pltpu.make_async_remote_copy(
            src_ref=pool_src.at[t, pl.ds(part - HALO, HALO)], dst_ref=pool_ref.at[pl.ds(0, HALO)],
            send_sem=h_send.at[t], recv_sem=h_recv.at[0], device_id=(sp + 1, t), device_id_type=MESH)

    def down_copy(t):
        return pltpu.make_async_remote_copy(
            src_ref=pool_src.at[t, pl.ds(0, HALO)], dst_ref=pool_ref.at[pl.ds(last, HALO)],
            send_sem=h_send.at[n_tp + t], recv_sem=h_recv.at[1], device_id=(sp - 1, t), device_id_type=MESH)

    sends_up = jnp.logical_and(tp == n_tp - 1, sp < n_sp - 1)
    sends_down = jnp.logical_and(tp == 0, sp > 0)

    @pl.when(sends_up)
    def _():
        for t in range(n_tp):
            up_copy(t).start()

    @pl.when(sends_down)
    def _():
        for t in range(n_tp):
            down_copy(t).start()

    @pl.when(sp == 0)
    def _():
        pool_ref[:HALO, :] = jnp.zeros((HALO, pool_cols), BF16)

    @pl.when(sp == n_sp - 1)
    def _():
        pool_ref[last:, :] = jnp.zeros((HALO, pool_cols), BF16)


    rows = n_tp * part
    heads = wqu_ref.shape[0] // HEAD
    pairs = q_s.shape[0] // 2
    lane = lax.broadcasted_iota(jnp.int32, (rows, 128), 1)

    def table(b):
        ca, sa = base_ref[:, :128], base_ref[:, 128:]
        cb, sb = block_ref[b, :, :128], block_ref[b, :, 128:]
        return ca * cb - sa * sb, sa * cb + ca * sb

    def relay(k):
        @pl.loop(0, n_ty)
        def _(j):
            i = k * n_ty + j

            @pl.when(i > 0)
            def _():
                slot = source_of(i)
                kv_copy(slot, part_send.at[i], (sp, partner)).wait_recv()
                kv_copy(slot, part_send.at[i], (sp, partner)).start()

    kg = row(kg_ref, 128)

    def build_keys(k):
        @pl.loop(0, n_ty)
        def _(j):
            i = k * n_ty + j
            slot = source_of(i) - core + 1 - core
            kv_copy(slot, part_send.at[i], (sp, partner)).wait_recv()

        b = lax.rem(sp + n_sp - k, n_sp)
        lat = jnp.concatenate([kv_ref[b * n_tp + t, :part, :] for t in range(n_tp)], axis=0)
        parts = []
        for t in range(n_tp):
            packed = kv_ref[b * n_tp + t, part:, :].astype(F32)
            for j in range(part // 16):
                parts.append(packed[:, j * ROT : (j + 1) * ROT])
        rope = jnp.concatenate(parts, axis=0)
        rope = jnp.concatenate([jnp.zeros((rows, PLAIN), F32), rope, jnp.zeros((rows, 128 - HEAD), F32)], axis=1)
        rope_sum = jnp.sum(rope * rope, axis=-1, keepdims=True)
        ck, sk = table(b)
        rotated = turn(rope * kg, ck, sk, lane)
        pair = mm(lat, wkvu_ref[...])
        at = pl.ds(pl.multiple_of(b * rows, 128), rows)
        for h in range(heads):
            kvh = pair[:, h * 128 : (h + 1) * 128]
            plain = jnp.where(lane < PLAIN, kvh, 0.0)
            r = lax.rsqrt((jnp.sum(plain * plain, axis=-1, keepdims=True) + rope_sum) * (1.0 / HEAD) + EPS)
            k_s[h, at, :] = (jnp.where(lane < PLAIN, kvh * kg, rotated) * r).astype(BF16)
            v_s[h, at, :] = jnp.where(lane < PLAIN, 1.0, kvh).astype(BF16)
        for h in range(heads, 2 * pairs):
            k_s[h, at, :] = jnp.zeros((rows, 128), BF16)
            v_s[h, at, :] = jnp.ones((rows, 128), BF16)

    relay(0)
    for i in range(1, n_tp):
        q_copy(i).wait_recv()
    cq, sq = table(sp)
    qg = row(qg_ref, 128) * np.float32(HEAD ** -0.5 * np.log2(np.e))
    ql = q_ref[...]
    for h in range(heads):
        w = jnp.concatenate(
            [wqu_ref[h * HEAD : (h + 1) * HEAD, :], jnp.zeros((128 - HEAD, wqu_ref.shape[1]), BF16)], axis=0)
        y = mm_t(ql, w)
        q_s[h] = turn(y * rms(y, HEAD) * qg, cq, sq, lane).astype(BF16)
    for h in range(heads, 2 * pairs):
        q_s[h] = jnp.zeros(q_s.shape[1:], BF16)

    @pl.loop(0, n_sp)
    def _(k):
        @pl.when(k < n_sp - 1)
        def _():
            relay(k + 1)

        build_keys(k)

    for i in range(1, n_tp):
        p_copy(i).wait_recv()

    def halo_wait(start, side):
        pltpu.make_async_remote_copy(
            src_ref=pool_src.at[0, pl.ds(0, HALO)], dst_ref=pool_ref.at[pl.ds(start, HALO)],
            send_sem=h_send.at[0], recv_sem=h_recv.at[side], device_id=(sp, partner),
            device_id_type=MESH).wait_recv()

    @pl.when(sp > 0)
    def _():
        halo_wait(0, 0)

    @pl.when(sp < n_sp - 1)
    def _():
        halo_wait(last, 1)

    x = pool_ref[...].astype(F32)
    size = x.shape[0]
    w1 = x + pltpu.roll(x, 1, 0)
    w2 = pltpu.roll(w1, 1, 0) + pltpu.roll(w1, size - 1, 0)
    w4 = pltpu.roll(w2, 2, 0) + pltpu.roll(w2, size - 2, 0)
    w8 = pltpu.roll(w4, 4, 0) + pltpu.roll(w4, size - 4, 0)
    x, w1, w2, w4, w8 = (v[HALO : HALO + rows] for v in (x, w1, w2, w4, w8))
    groups_here = mix_ref.shape[0]
    wide = x.shape[1]
    kind = lax.rem(tp * groups_here + lane[:, :wide] // GDIM, 4)
    window = jnp.where(kind == 0, w1, jnp.where(kind == 1, w2, jnp.where(kind == 2, w4, w8)))
    half = jnp.where(kind == 0, 1, jnp.where(kind == 1, 2, jnp.where(kind == 2, 4, 8)))
    place = sp * rows + lax.broadcasted_iota(jnp.int32, (rows, wide), 0)
    count = (jnp.minimum(place + half, rows * n_sp) - jnp.maximum(place - half, 0)).astype(F32)
    pooled = (window / count - x).astype(BF16)
    mapped = jnp.concatenate(
        [mm(pooled[:, g * GDIM : (g + 1) * GDIM], mix_ref[g]) for g in range(groups_here)], axis=1)
    cat_s[...] = (mapped * row(scale_ref)).astype(BF16)

    chunk = 2 * part
    lane_c = lax.broadcasted_iota(jnp.int32, (chunk, 128), 1)
    tile = 512
    width = out_ref.shape[1]
    span = width // pieces

    def cols(p):
        return pl.ds(p * span, span)

    def one_head(h, at):
        s = mm_t(q_s[h, at, :], k_s[h])
        m = jnp.max(s, axis=-1, keepdims=True)
        p = jnp.exp2(s - m).astype(BF16)
        o = mm(p, v_s[h])
        total = o[:, :1]
        lse = m * np.float32(np.log(2.0)) + jnp.log(total)
        return o * (1.0 / total), lse

    def d_copy(i, p):
        return pltpu.make_async_remote_copy(
            src_ref=part_s.at[i, 1 - core, :, cols(p)], dst_ref=from_partner.at[i, :, cols(p)],
            send_sem=d_send.at[i * pieces + p], recv_sem=d_recv.at[i * pieces + p],
            device_id=(sp, partner), device_id_type=MESH)

    def c_copy(i, p):
        return pltpu.make_async_remote_copy(
            src_ref=to_send.at[i, :, cols(p)], dst_ref=from_chip.at[i, :, cols(p)],
            send_sem=c_send.at[i * pieces + p], recv_sem=c_recv.at[i * pieces + p],
            device_id=(sp, lax.rem(ty + i, n_ty) * 2 + core), device_id_type=MESH)

    @pl.loop(0, n_ty * pairs)
    def _(step):
        turn_no = step // pairs
        j = lax.rem(step, pairs)
        i = lax.rem(turn_no + 1, n_ty)
        at = pl.ds(pl.multiple_of(lax.rem(ty + i, n_ty) * chunk, 32), chunk)
        even, lse0 = one_head(2 * j, at)
        odd, lse1 = one_head(2 * j + 1, at)
        both = jnp.where(lane_c < VALUE, pltpu.roll(even, VALUE, 1), odd).astype(BF16)
        att_s[j, :, :] = both
        lse_ref[pl.ds(j, 1), pl.ds(lax.rem(ty + i, n_ty), 1), :, :] = jnp.transpose(
            jnp.concatenate([lse0, lse1], axis=1))[None, None]

        @pl.when(jnp.logical_and(j == 0, turn_no > 0))
        def _():
            for p in range(pieces):
                d_copy(turn_no, p).wait_recv()
                to_send[turn_no, :, cols(p)] = (
                    part_s[turn_no, core, :, cols(p)].astype(F32)
                    + from_partner[turn_no, :, cols(p)].astype(F32)).astype(BF16)
                c_copy(turn_no, p).start()

        @pl.when(j == pairs - 1)
        def _():
            attention = jnp.concatenate([att_s[p] for p in range(pairs)], axis=1)[:, : heads * VALUE]
            pool_out = cat_s[at, :]

            for p in range(pieces):
                for n in range(span // tile):
                    cc = pl.ds(p * span + n * tile, tile)
                    y = (mm(attention, woa_ref[:, cc]) + mm(pool_out, wop_ref[:, cc])).astype(BF16)
                    part_s[i, :, :, cc] = y.reshape(2, part, tile)
                d_copy(i, p).start()

    for p in range(pieces):
        d_copy(0, p).wait_recv()
        total = part_s[0, core, :, cols(p)].astype(F32) + from_partner[0, :, cols(p)].astype(F32)
        for i in range(1, n_ty):
            c_copy(i, p).wait_recv()
            total = total + from_chip[i, :, cols(p)].astype(F32)
        out_ref[:, cols(p)] = total.astype(BF16)

    for i in range(n_ty):
        for p in range(pieces):
            d_copy(i, p).wait_send()
            if i:
                c_copy(i, p).wait_send()
    for i in range(1, n_tp):
        q_copy(i).wait_send()
        p_copy(i).wait_send()

    @pl.when(sends_up)
    def _():
        for t in range(n_tp):
            up_copy(t).wait_send()

    @pl.when(sends_down)
    def _():
        for t in range(n_tp):
            down_copy(t).wait_send()

    @pl.loop(1, n_chip)
    def _(i):
        kv_copy(me, kv_send.at[i], chip_of(i)).wait_send()

    @pl.loop(0, n_chip)
    def _(i):
        kv_copy(me, part_send.at[i], (sp, partner)).wait_send()


def tables(rows, blocks):
    half = ROT // 2
    freqs = ROPE_BASE ** (-np.arange(half, dtype=np.float64) / half)

    def make(positions):
        angle = positions[:, None] * freqs[None, :]
        out = np.zeros((len(positions), 256), np.float64)
        out[:, :PLAIN] = 1.0
        out[:, PLAIN:HEAD] = np.concatenate([np.cos(angle), np.cos(angle)], axis=1)
        out[:, 128 + PLAIN : 128 + HEAD] = np.concatenate([-np.sin(angle), np.sin(angle)], axis=1)
        return out.astype(np.float32)

    return make(np.arange(rows)), make(np.arange(blocks) * rows)[:, None]


def shards(n_sp, n_tp, tokens, norm_gain, wq, q_lat_gain, wkv, kv_lat_gain, w_rope, w_pool_in, wqu, wkvu,
           query_gain, key_gain, w_mix, pool_scale, w_out_attn, w_out_pool):
    part, width = tokens.shape
    rows = part * n_tp
    total = rows * n_sp
    heads = wqu.shape[1] // HEAD
    pairs = (heads + 1) // 2
    pool_cols = w_mix.shape[0] * GDIM
    n_dev = n_sp * n_tp
    n_ty = n_tp // 2
    n_chip = n_dev // 2
    pieces = 2
    dma = pltpu.SemaphoreType.DMA
    rank = wkv.shape[1]
    base, block = tables(rows, n_sp)
    mixed, lse = pl.pallas_call(
        functools.partial(layer_kernel, n_sp, n_tp, pieces),
        out_shape=[
            jax.ShapeDtypeStruct((part, width), BF16),
            jax.ShapeDtypeStruct((pairs, n_ty, 2, 2 * part), F32),
        ],
        in_specs=[VMEM] * 18,
        out_specs=[VMEM] * 2,
        scratch_shapes=[
            pltpu.VMEM((rows, wq.shape[1]), BF16),
            pltpu.VMEM((rows + 2 * HALO, pool_cols), BF16),
            pltpu.VMEM((n_dev, part + 16, rank), BF16),
            pltpu.VMEM((n_tp, part, pool_cols), BF16),
            pltpu.VMEM((2 * pairs, rows, 128), BF16),
            pltpu.VMEM((2 * pairs, total, 128), BF16),
            pltpu.VMEM((2 * pairs, total, 128), BF16),
            pltpu.VMEM((rows, pool_cols), BF16),
            pltpu.VMEM((pairs, 2 * part, 128), BF16),
            pltpu.VMEM((n_ty, 2, part, width), BF16),
            pltpu.VMEM((n_ty, part, width), BF16),
            pltpu.VMEM((n_ty, part, width), BF16),
            pltpu.VMEM((n_ty, part, width), BF16),
            dma((n_chip,)), dma((n_dev,)), dma((n_chip,)),
            dma((n_tp,)), dma((n_tp,)), dma((n_tp,)), dma((n_tp,)), dma((2 * n_tp,)), dma((2,)),
            dma((n_ty * pieces,)), dma((n_ty * pieces,)), dma((n_ty * pieces,)), dma((n_ty * pieces,)),
        ],
        compiler_params=pltpu.CompilerParams(
            collective_id=0, has_side_effects=True, vmem_limit_bytes=63 * 2**20),
    )(tokens, norm_gain, wq, q_lat_gain, wkv, kv_lat_gain, w_rope.T, w_pool_in,
      wqu.T, wkvu, query_gain, key_gain, w_mix, pool_scale, w_out_attn, w_out_pool, base, block)
    return mixed, jnp.transpose(lse, (0, 2, 1, 3)).reshape(2 * pairs, rows)[:heads]


def solution(mesh):
    placed = (
        P(("sp", "tp"), None), P(), P(), P(), P(), P(), P(), P(),
        P(None, "tp"), P(None, "tp"), P(), P(),
        P("tp", None, None), P("tp"), P("tp", None), P("tp", None),
    )
    return jax.shard_map(
        functools.partial(shards, mesh.shape["sp"], mesh.shape["tp"]),
        mesh=mesh,
        in_specs=placed,
        out_specs=(P(("sp", "tp"), None), P("tp", "sp")),
        check_vma=False,
    )
```

```python
import functools

import jax
import jax.numpy as jnp
import numpy as np
from jax import lax
from jax.experimental import pallas as pl
from jax.experimental.pallas import tpu as pltpu
from jax.sharding import PartitionSpec as P

PLAIN = 64
ROT = 32
HEAD = PLAIN + ROT
VALUE = 64
GDIM = 64
EPS = 1e-06
ROPE_BASE = 10000.0
HALO = 16
F32 = jnp.float32
BF16 = jnp.bfloat16
MESH = pl.DeviceIdType.MESH
VMEM = pl.BlockSpec(memory_space=pltpu.VMEM)


def rms(x, width):
    return lax.rsqrt(jnp.sum(x * x, axis=-1, keepdims=True) * (1.0 / width) + EPS)


def row(ref, width=None):
    v = ref[...].astype(F32).reshape(1, ref.shape[0])
    if width and width > ref.shape[0]:
        v = jnp.concatenate([v, jnp.zeros((1, width - ref.shape[0]), F32)], axis=1)
    return v


def mm_t(a, b):
    return lax.dot_general(a, b, (((1,), (1,)), ((), ())), preferred_element_type=F32)


def mm(a, b):
    return jnp.dot(a, b, preferred_element_type=F32)


def turn(y, cosine, sine, lane):
    half = ROT // 2
    width = y.shape[-1]
    swapped = jnp.where(lane < PLAIN + half, pltpu.roll(y, width - half, 1), pltpu.roll(y, half, 1))
    return y * cosine + swapped * sine


def layer_kernel(n_sp, n_tp, n_x, pieces, x_ref, gain_ref, wq_hbm, qlg_ref, wkv_ref, kvg_ref, wr_ref, wp_hbm,
                 wqu_hbm, wkvu_hbm, qg_ref, kg_ref, mix_ref, scale_ref, woa_hbm, wop_hbm, base_ref, block_ref,
                 out_ref, lse_ref,
                 wq_ref, wp_ref, wqu_ref, wkvu_ref, woa_ref, wop_ref, w_sem,
                 q_ref, pool_ref, kv_ref, pool_src, q_s, k_s, v_s, cat_s, att_s, part_s, from_partner, to_send, from_chip,
                 z_send, y_send, x_send, kv_recv, part_send, q_send, q_recv, p_send, p_recv, h_send, h_recv,
                 d_send, d_recv, c_send, c_recv):
    sp = lax.axis_index("sp")
    tp = lax.axis_index("tp")
    n_dev = n_sp * n_tp
    n_ty = n_tp // 2
    n_chip = n_sp * n_ty
    n_z = n_sp // n_x
    me = sp * n_tp + tp
    core = lax.rem(tp, 2)
    ty = tp // 2
    partner = ty * 2 + 1 - core
    part = x_ref.shape[0]
    pool_cols = pool_ref.shape[1]
    loads = [
        pltpu.make_async_copy(source, target, w_sem.at[n])
        for n, (source, target) in enumerate([
            (wq_hbm, wq_ref), (wp_hbm, wp_ref), (wqu_hbm, wqu_ref),
            (wkvu_hbm, wkvu_ref), (woa_hbm, woa_ref), (wop_hbm, wop_ref)])
    ]
    for load in loads:
        load.start()
    barrier = pltpu.get_barrier_semaphore()

    @pl.loop(1, n_dev)
    def _(i):
        d = lax.rem(me + i, n_dev)
        pl.semaphore_signal(barrier, inc=1, device_id=(d // n_tp, lax.rem(d, n_tp)), device_id_type=MESH)

    x = x_ref[...].astype(F32)
    normed = (x * rms(x, x.shape[1]) * row(gain_ref)).astype(BF16)
    kv = mm(normed, wkv_ref[...])
    kv_ref[me, :part, :] = (kv * rms(kv, kv.shape[1]) * row(kvg_ref)).astype(BF16)
    rope = mm_t(normed, wr_ref[...])
    groups = part // 16
    packed = [rope[16 * j : 16 * j + 16, :] for j in range(groups)]
    packed.append(jnp.zeros((16, kv.shape[1] - groups * ROT), F32))
    kv_ref[me, part:, :] = jnp.concatenate(packed, axis=1).astype(BF16)
    pl.semaphore_wait(barrier, n_dev - 1)

    x_of, z_of = lax.rem(sp, n_x), sp // n_x

    def block_of(dx, dz):
        return lax.rem(z_of + n_z - dz, n_z) * n_x + lax.rem(x_of + n_x - dx, n_x)

    def slot_of(dx, dy, dz):
        return block_of(dx, dz) * n_tp + lax.rem(ty + n_ty - dy, n_ty) * 2 + core

    def kv_copy(slot, send_sem, target):
        return pltpu.make_async_remote_copy(
            src_ref=kv_ref.at[slot], dst_ref=kv_ref.at[slot], send_sem=send_sem,
            recv_sem=kv_recv.at[slot], device_id=target, device_id_type=MESH)

    def z_copy(i):
        return kv_copy(me, z_send.at[i], (lax.rem(z_of + i, n_z) * n_x + x_of, tp))

    def y_copy(slot, dz, i):
        return kv_copy(slot, y_send.at[dz * n_ty + i], (sp, lax.rem(ty + i, n_ty) * 2 + core))

    def x_copy(slot, dy, dz, i):
        return kv_copy(slot, x_send.at[(dz * n_ty + dy) * n_x + i], (z_of * n_x + lax.rem(x_of + i, n_x), tp))

    def to_partner(slot, dx, dy, dz):
        return kv_copy(slot, part_send.at[(dx * n_z + dz) * n_ty + dy], (sp, partner))

    def spread(dy, dz):
        slot = slot_of(0, dy, dz)

        @pl.when(dy + dz > 0)
        def _():
            z_wait(slot)

        if isinstance(dy, int):
            for i in range(1, n_ty):
                y_copy(slot, dz, i).start()
        for i in range(1, n_x):
            x_copy(slot, dy, dz, i).start()
        to_partner(slot, 0, dy, dz).start()

    def z_wait(slot):
        kv_copy(slot, part_send.at[0], (sp, partner)).wait_recv()

    for i in range(1, n_z):
        z_copy(i).start()

    spread(0, jnp.int32(0))

    loads[0].wait()
    q = mm(normed, wq_ref[...])
    q_rows = pl.ds(pl.multiple_of(tp * part, 16), part)
    q_ref[q_rows, :] = (q * rms(q, q.shape[1]) * row(qlg_ref)).astype(BF16)

    def q_copy(i):
        return pltpu.make_async_remote_copy(
            src_ref=q_ref.at[q_rows], dst_ref=q_ref.at[q_rows], send_sem=q_send.at[i],
            recv_sem=q_recv.at[i], device_id=(sp, lax.rem(tp + i, n_tp)), device_id_type=MESH)

    for i in range(1, n_tp):
        q_copy(i).start()
    loads[1].wait()
    pool = mm(normed, wp_ref[...]).astype(BF16)
    for t in range(n_tp):
        pool_src[t] = pool[:, t * pool_cols : (t + 1) * pool_cols]
    pool_ref[pl.ds(pl.multiple_of(HALO + tp * part, 16), part), :] = pool_src[tp]

    def p_copy(i):
        t = lax.rem(tp + i, n_tp)
        return pltpu.make_async_remote_copy(
            src_ref=pool_src.at[t],
            dst_ref=pool_ref.at[pl.ds(pl.multiple_of(HALO + tp * part, 16), part)],
            send_sem=p_send.at[i], recv_sem=p_recv.at[i],
            device_id=(sp, t), device_id_type=MESH)

    for i in range(1, n_tp):
        p_copy(i).start()
    last = HALO + n_tp * part

    def up_copy(t):
        return pltpu.make_async_remote_copy(
            src_ref=pool_src.at[t, pl.ds(part - HALO, HALO)], dst_ref=pool_ref.at[pl.ds(0, HALO)],
            send_sem=h_send.at[t], recv_sem=h_recv.at[0], device_id=(sp + 1, t), device_id_type=MESH)

    def down_copy(t):
        return pltpu.make_async_remote_copy(
            src_ref=pool_src.at[t, pl.ds(0, HALO)], dst_ref=pool_ref.at[pl.ds(last, HALO)],
            send_sem=h_send.at[n_tp + t], recv_sem=h_recv.at[1], device_id=(sp - 1, t), device_id_type=MESH)

    sends_up = jnp.logical_and(tp == n_tp - 1, sp < n_sp - 1)
    sends_down = jnp.logical_and(tp == 0, sp > 0)

    @pl.when(sends_up)
    def _():
        for t in range(n_tp):
            up_copy(t).start()

    @pl.when(sends_down)
    def _():
        for t in range(n_tp):
            down_copy(t).start()

    @pl.when(sp == 0)
    def _():
        pool_ref[:HALO, :] = jnp.zeros((HALO, pool_cols), BF16)

    @pl.when(sp == n_sp - 1)
    def _():
        pool_ref[last:, :] = jnp.zeros((HALO, pool_cols), BF16)


    rows = n_tp * part
    heads = wqu_ref.shape[0] // HEAD
    pairs = q_s.shape[0] // 2
    lane = lax.broadcasted_iota(jnp.int32, (rows, 128), 1)

    def table(b):
        ca, sa = base_ref[:, :128], base_ref[:, 128:]
        cb, sb = block_ref[b, :, :128], block_ref[b, :, 128:]
        return ca * cb - sa * sb, sa * cb + ca * sb

    def relay(k):
        @pl.loop(0, n_ty)
        def _(dy):
            slot = slot_of(k // n_z, dy, lax.rem(k, n_z))
            z_wait(slot)
            to_partner(slot, k // n_z, dy, lax.rem(k, n_z)).start()

    kg = row(kg_ref, 128)

    def build_keys(k):
        @pl.loop(0, n_ty)
        def _(j):
            z_wait(slot_of(k // n_z, j, lax.rem(k, n_z)) - core + 1 - core)

        b = block_of(k // n_z, lax.rem(k, n_z))
        lat = jnp.concatenate([kv_ref[b * n_tp + t, :part, :] for t in range(n_tp)], axis=0)
        parts = []
        for t in range(n_tp):
            packed = kv_ref[b * n_tp + t, part:, :].astype(F32)
            for j in range(part // 16):
                parts.append(packed[:, j * ROT : (j + 1) * ROT])
        rope = jnp.concatenate(parts, axis=0)
        rope = jnp.concatenate([jnp.zeros((rows, PLAIN), F32), rope, jnp.zeros((rows, 128 - HEAD), F32)], axis=1)
        rope_sum = jnp.sum(rope * rope, axis=-1, keepdims=True)
        ck, sk = table(b)
        rotated = turn(rope * kg, ck, sk, lane)
        pair = mm(lat, wkvu_ref[...])
        at = pl.ds(pl.multiple_of(b * rows, 128), rows)
        for h in range(heads):
            kvh = pair[:, h * 128 : (h + 1) * 128]
            plain = jnp.where(lane < PLAIN, kvh, 0.0)
            r = lax.rsqrt((jnp.sum(plain * plain, axis=-1, keepdims=True) + rope_sum) * (1.0 / HEAD) + EPS)
            k_s[h, at, :] = (jnp.where(lane < PLAIN, kvh * kg, rotated) * r).astype(BF16)
            v_s[h, at, :] = jnp.where(lane < PLAIN, 1.0, kvh).astype(BF16)
        for h in range(heads, 2 * pairs):
            k_s[h, at, :] = jnp.zeros((rows, 128), BF16)
            v_s[h, at, :] = jnp.ones((rows, 128), BF16)

    @pl.loop(1, n_z)
    def _(dz):
        spread(0, dz)

    for i in range(1, n_tp):
        q_copy(i).wait_recv()
    for load in loads[2:]:
        load.wait()
    cq, sq = table(sp)
    qg = row(qg_ref, 128) * np.float32(HEAD ** -0.5 * np.log2(np.e))
    ql = q_ref[...]
    for h in range(heads):
        w = jnp.concatenate(
            [wqu_ref[h * HEAD : (h + 1) * HEAD, :], jnp.zeros((128 - HEAD, wqu_ref.shape[1]), BF16)], axis=0)
        y = mm_t(ql, w)
        q_s[h] = turn(y * rms(y, HEAD) * qg, cq, sq, lane).astype(BF16)
    for h in range(heads, 2 * pairs):
        q_s[h] = jnp.zeros(q_s.shape[1:], BF16)

    @pl.loop(0, n_z * (n_ty - 1))
    def _(i):
        spread(1 + i // n_z, lax.rem(i, n_z))

    @pl.loop(0, n_sp)
    def _(k):
        @pl.when(jnp.logical_and(k + 1 >= n_z, k < n_sp - 1))
        def _():
            relay(k + 1)

        build_keys(k)

    for i in range(1, n_tp):
        p_copy(i).wait_recv()

    def halo_wait(start, side):
        pltpu.make_async_remote_copy(
            src_ref=pool_src.at[0, pl.ds(0, HALO)], dst_ref=pool_ref.at[pl.ds(start, HALO)],
            send_sem=h_send.at[0], recv_sem=h_recv.at[side], device_id=(sp, partner),
            device_id_type=MESH).wait_recv()

    @pl.when(sp > 0)
    def _():
        halo_wait(0, 0)

    @pl.when(sp < n_sp - 1)
    def _():
        halo_wait(last, 1)

    x = pool_ref[...].astype(F32)
    size = x.shape[0]
    w1 = x + pltpu.roll(x, 1, 0)
    w2 = pltpu.roll(w1, 1, 0) + pltpu.roll(w1, size - 1, 0)
    w4 = pltpu.roll(w2, 2, 0) + pltpu.roll(w2, size - 2, 0)
    w8 = pltpu.roll(w4, 4, 0) + pltpu.roll(w4, size - 4, 0)
    x, w1, w2, w4, w8 = (v[HALO : HALO + rows] for v in (x, w1, w2, w4, w8))
    groups_here = mix_ref.shape[0]
    wide = x.shape[1]
    kind = lax.rem(tp * groups_here + lane[:, :wide] // GDIM, 4)
    window = jnp.where(kind == 0, w1, jnp.where(kind == 1, w2, jnp.where(kind == 2, w4, w8)))
    half = jnp.where(kind == 0, 1, jnp.where(kind == 1, 2, jnp.where(kind == 2, 4, 8)))
    place = sp * rows + lax.broadcasted_iota(jnp.int32, (rows, wide), 0)
    count = (jnp.minimum(place + half, rows * n_sp) - jnp.maximum(place - half, 0)).astype(F32)
    pooled = (window / count - x).astype(BF16)
    mapped = jnp.concatenate(
        [mm(pooled[:, g * GDIM : (g + 1) * GDIM], mix_ref[g]) for g in range(groups_here)], axis=1)
    cat_s[...] = (mapped * row(scale_ref)).astype(BF16)

    chunk = 2 * part
    lane_c = lax.broadcasted_iota(jnp.int32, (chunk, 128), 1)
    tile = 512
    width = out_ref.shape[1]
    span = width // pieces

    def cols(p):
        return pl.ds(p * span, span)

    def finish(s, m, h):
        p = jnp.exp2(s - m).astype(BF16)
        o = mm(p, v_s[h])
        total = o[:, :1]
        lse = m * np.float32(np.log(2.0)) + jnp.log(total)
        return o * (1.0 / total), lse

    def d_copy(i, p):
        return pltpu.make_async_remote_copy(
            src_ref=part_s.at[i, 1 - core, :, cols(p)], dst_ref=from_partner.at[i, :, cols(p)],
            send_sem=d_send.at[i * pieces + p], recv_sem=d_recv.at[i * pieces + p],
            device_id=(sp, partner), device_id_type=MESH)

    def c_copy(i, p):
        return pltpu.make_async_remote_copy(
            src_ref=to_send.at[i, :, cols(p)], dst_ref=from_chip.at[i, :, cols(p)],
            send_sem=c_send.at[i * pieces + p], recv_sem=c_recv.at[i * pieces + p],
            device_id=(sp, lax.rem(ty + i, n_ty) * 2 + core), device_id_type=MESH)

    @pl.loop(0, n_ty * pairs)
    def _(step):
        turn_no = step // pairs
        j = lax.rem(step, pairs)
        i = lax.rem(turn_no + 1, n_ty)
        at = pl.ds(pl.multiple_of(lax.rem(ty + i, n_ty) * chunk, 32), chunk)
        s0 = mm_t(q_s[2 * j, at, :], k_s[2 * j])
        m0 = jnp.max(s0, axis=-1, keepdims=True)
        s1 = mm_t(q_s[2 * j + 1, at, :], k_s[2 * j + 1])
        m1 = jnp.max(s1, axis=-1, keepdims=True)
        even, lse0 = finish(s0, m0, 2 * j)
        odd, lse1 = finish(s1, m1, 2 * j + 1)
        both = jnp.where(lane_c < VALUE, pltpu.roll(even, VALUE, 1), odd).astype(BF16)
        att_s[j, :, :] = both
        lse_ref[pl.ds(j, 1), pl.ds(lax.rem(ty + i, n_ty), 1), :, :] = jnp.transpose(
            jnp.concatenate([lse0, lse1], axis=1))[None, None]

        @pl.when(jnp.logical_and(j == 0, turn_no > 0))
        def _():
            for p in range(pieces):
                d_copy(turn_no, p).wait_recv()
                to_send[turn_no, :, cols(p)] = (
                    part_s[turn_no, core, :, cols(p)].astype(F32)
                    + from_partner[turn_no, :, cols(p)].astype(F32)).astype(BF16)
                c_copy(turn_no, p).start()

        @pl.when(j == pairs - 1)
        def _():
            attention = jnp.concatenate([att_s[p] for p in range(pairs)], axis=1)[:, : heads * VALUE]
            pool_out = cat_s[at, :]

            for p in range(pieces):
                for n in range(span // tile):
                    cc = pl.ds(p * span + n * tile, tile)
                    y = (mm(attention, woa_ref[:, cc]) + mm(pool_out, wop_ref[:, cc])).astype(BF16)
                    part_s[i, :, :, cc] = y.reshape(2, part, tile)
                d_copy(i, p).start()

    for p in range(pieces):
        d_copy(0, p).wait_recv()
        total = part_s[0, core, :, cols(p)].astype(F32) + from_partner[0, :, cols(p)].astype(F32)
        for i in range(1, n_ty):
            c_copy(i, p).wait_recv()
            total = total + from_chip[i, :, cols(p)].astype(F32)
        out_ref[:, cols(p)] = total.astype(BF16)

    for i in range(n_ty):
        for p in range(pieces):
            d_copy(i, p).wait_send()
            if i:
                c_copy(i, p).wait_send()
    for i in range(1, n_tp):
        q_copy(i).wait_send()
        p_copy(i).wait_send()

    @pl.when(sends_up)
    def _():
        for t in range(n_tp):
            up_copy(t).wait_send()

    @pl.when(sends_down)
    def _():
        for t in range(n_tp):
            down_copy(t).wait_send()

    for i in range(1, n_z):
        z_copy(i).wait_send()

    @pl.loop(0, n_z)
    def _(dz):
        for i in range(1, n_ty):
            y_copy(me, dz, i).wait_send()

        @pl.loop(0, n_ty)
        def _(dy):
            for i in range(1, n_x):
                x_copy(me, dy, dz, i).wait_send()

    @pl.loop(0, n_chip)
    def _(i):
        kv_copy(me, part_send.at[i], (sp, partner)).wait_send()


def tables(rows, blocks):
    half = ROT // 2
    freqs = ROPE_BASE ** (-np.arange(half, dtype=np.float64) / half)

    def make(positions):
        angle = positions[:, None] * freqs[None, :]
        out = np.zeros((len(positions), 256), np.float64)
        out[:, :PLAIN] = 1.0
        out[:, PLAIN:HEAD] = np.concatenate([np.cos(angle), np.cos(angle)], axis=1)
        out[:, 128 + PLAIN : 128 + HEAD] = np.concatenate([-np.sin(angle), np.sin(angle)], axis=1)
        return out.astype(np.float32)

    return make(np.arange(rows)), make(np.arange(blocks) * rows)[:, None]


def shards(n_sp, n_tp, tokens, norm_gain, wq, q_lat_gain, wkv, kv_lat_gain, w_rope, w_pool_in, wqu, wkvu,
           query_gain, key_gain, w_mix, pool_scale, w_out_attn, w_out_pool):
    part, width = tokens.shape
    rows = part * n_tp
    total = rows * n_sp
    heads = wqu.shape[1] // HEAD
    pairs = (heads + 1) // 2
    pool_cols = w_mix.shape[0] * GDIM
    n_dev = n_sp * n_tp
    n_ty = n_tp // 2
    n_chip = n_dev // 2
    n_x = 2 ** ((n_sp.bit_length() - 1) // 2)
    n_x = n_x if n_sp % n_x == 0 else 1
    n_z = n_sp // n_x
    pieces = 2
    dma = pltpu.SemaphoreType.DMA
    rank = wkv.shape[1]
    base, block = tables(rows, n_sp)
    mixed, lse = pl.pallas_call(
        functools.partial(layer_kernel, n_sp, n_tp, n_x, pieces),
        out_shape=[
            jax.ShapeDtypeStruct((part, width), BF16),
            jax.ShapeDtypeStruct((pairs, n_ty, 2, 2 * part), F32),
        ],
        in_specs=[VMEM if n not in (2, 7, 8, 9, 14, 15) else pl.BlockSpec(memory_space=pl.ANY) for n in range(18)],
        out_specs=[VMEM] * 2,
        scratch_shapes=[
            pltpu.VMEM(wq.shape, BF16),
            pltpu.VMEM(w_pool_in.shape, BF16),
            pltpu.VMEM(wqu.shape[::-1], BF16),
            pltpu.VMEM(wkvu.shape, BF16),
            pltpu.VMEM(w_out_attn.shape, BF16),
            pltpu.VMEM(w_out_pool.shape, BF16),
            dma((6,)),
            pltpu.VMEM((rows, wq.shape[1]), BF16),
            pltpu.VMEM((rows + 2 * HALO, pool_cols), BF16),
            pltpu.VMEM((n_dev, part + 16, rank), BF16),
            pltpu.VMEM((n_tp, part, pool_cols), BF16),
            pltpu.VMEM((2 * pairs, rows, 128), BF16),
            pltpu.VMEM((2 * pairs, total, 128), BF16),
            pltpu.VMEM((2 * pairs, total, 128), BF16),
            pltpu.VMEM((rows, pool_cols), BF16),
            pltpu.VMEM((pairs, 2 * part, 128), BF16),
            pltpu.VMEM((n_ty, 2, part, width), BF16),
            pltpu.VMEM((n_ty, part, width), BF16),
            pltpu.VMEM((n_ty, part, width), BF16),
            pltpu.VMEM((n_ty, part, width), BF16),
            dma((n_z,)), dma((n_z * n_ty,)), dma((n_chip * n_x,)), dma((n_dev,)), dma((n_chip,)),
            dma((n_tp,)), dma((n_tp,)), dma((n_tp,)), dma((n_tp,)), dma((2 * n_tp,)), dma((2,)),
            dma((n_ty * pieces,)), dma((n_ty * pieces,)), dma((n_ty * pieces,)), dma((n_ty * pieces,)),
        ],
        compiler_params=pltpu.CompilerParams(
            collective_id=0, has_side_effects=True, vmem_limit_bytes=63 * 2**20),
    )(tokens, norm_gain, wq, q_lat_gain, wkv, kv_lat_gain, w_rope.T, w_pool_in,
      wqu.T, wkvu, query_gain, key_gain, w_mix, pool_scale, w_out_attn, w_out_pool, base, block)
    return mixed, jnp.transpose(lse, (0, 2, 1, 3)).reshape(2 * pairs, rows)[:heads]


def solution(mesh):
    placed = (
        P(("sp", "tp"), None), P(), P(), P(), P(), P(), P(), P(),
        P(None, "tp"), P(None, "tp"), P(), P(),
        P("tp", None, None), P("tp"), P("tp", None), P("tp", None),
    )
    return jax.shard_map(
        functools.partial(shards, mesh.shape["sp"], mesh.shape["tp"]),
        mesh=mesh,
        in_specs=placed,
        out_specs=(P(("sp", "tp"), None), P("tp", "sp")),
        check_vma=False,
    )
```
